32 devices in a mesh: sp: 8 (over z, y), tp: 4 (over x, core).
Axes of the slice: x: 2, y: 2, z: 4, core: 2. Of those that a mesh axis runs over, the one named last changes fastest.
Arguments:
- pooled_in: bfloat16 [8192, 2048], P('sp', 'tp'), may hold values from -6 to 6
- group_map: bfloat16 [4, 512, 512], P('tp'), may hold values from -0.25 to 0.25
- pool_scale: float32 [2048], P('tp'), may hold values from 0.1 to 1.9
- out_weight: bfloat16 [2048, 2048], P('tp'), may hold values from -0.125 to 0.125
- residual: bfloat16 [8192, 2048], P(('sp', 'tp')), may hold values from -6 to 6
- norm_gain: float32 [2048], replicated, may hold values from 0.1 to 1.9
- gate_weight: bfloat16 [8, 2048, 512], P('sp'), may hold values from -0.125 to 0.125
- up_weight: bfloat16 [8, 2048, 512], P('sp'), may hold values from -0.125 to 0.125
- down_weight: bfloat16 [8, 512, 2048], P('sp'), may hold values from -0.25 to 0.25
- route_expert: int32 [8192, 2], P(('sp', 'tp')), may hold values from 0 to 7, all different within a row; in each aligned block of 256 rows (0 to 255, 256 to 511, ...) at most 96 rows name the same one
- route_score: float32 [8192, 2], P(('sp', 'tp')), may hold values from 0.05 to 1
Outputs:
- layer_out: bfloat16 [8192, 2048], P(('sp', 'tp'))
The draws below stay inside these ranges and needn't reach their ends.
Inputs may be any that keep to these rules, and one draw needn't show every extreme that they name: `route_expert`: each token names 2 different experts. Within each aligned block of 256 tokens (the rows of one device) no expert is named by more than 96 tokens, and in some such block one expert is named by exactly 96.
All inputs are finite; a program needn't handle non-finite values.
Results may differ from the reference program's by a relative error of at most 0.0065.
Values may be sent and summed in bfloat16 or wider, within the bound.
No kernel may reach another device: no remote copies, remote signals or barrier semaphores. Data moves between devices by JAX's collectives and lax.ppermute only.
A program may use at most 64 MiB of HBM per device.

```python
import math
import jax
import jax.numpy as jnp
import numpy as np
from jax import lax

D = 2048
GROUPS = 4
D_POOL = 2048
GROUP = 512
FF = 512
TOP = 2
ROWS_DEV = 256
TOKENS = 8192
EXPERTS = 8
CAP = 96


def block_scale(own_key, shape, split, least, largest):
    gain = 1.0
    for axis_at, shards_of in split:
        draws = jax.random.uniform(jax.random.fold_in(jax.random.fold_in(own_key, 6), axis_at), (shards_of,), jnp.float32, least / len(split), largest / len(split))
        gain = gain * jnp.repeat(jnp.exp(draws), shape[axis_at] // shards_of).reshape((-1,) + (1,) * (len(shape) - 1 - axis_at))
    return gain


def routed_block(stream_key, own, number, rows, count, top, limit, lean):
    order = jax.random.permutation(stream_key, count)
    heavy_load, usual = shares(count, rows * top, limit, lean, True), shares(count, rows * top, limit, lean, False)
    places = jnp.arange(count)

    def named(tallies, rotation):
        used = int((tallies > 0).sum())
        fixed = max(1, used // 4)
        shifted = fixed + (places - fixed + rotation * (used - fixed)) % max(1, count - fixed)
        return jnp.zeros((count,), jnp.int32).at[order[jnp.where(places < fixed, places, shifted)]].set(jnp.asarray(tallies, jnp.int32))

    tallies = jnp.where(number % 4 == 0, named(heavy_load, number // 4), named(usual, number - number // 4 - 1))
    mixed = jax.random.permutation(jax.random.fold_in(own, 3), count)
    source_of, taker = mixed[0:count // 2 * 2:2], mixed[1:count // 2 * 2:2]
    slack = jnp.minimum(tallies[source_of] - 1, limit - tallies[taker]) // 2
    slack = jnp.where((source_of == order[0]) | (taker == order[0]) | (tallies[taker] == 0), 0, jnp.maximum(slack, 0))
    shifted = jax.random.randint(jax.random.fold_in(own, 4), (count // 2,), 0, 1 << 20) % (slack + 1)
    tallies = tallies.at[source_of].add(-shifted).at[taker].add(shifted)
    labels = jnp.searchsorted(jnp.cumsum(tallies), jnp.arange(rows * top), side="right").astype(jnp.int32)
    table = labels.reshape(top, rows).T
    table = table[jax.random.permutation(jax.random.fold_in(own, 1), rows)]
    rotation = jax.random.randint(jax.random.fold_in(own, 2), (rows, 1), 0, top)
    return jnp.take_along_axis(table, (jnp.arange(top)[None, :] + rotation) % top, axis=1)


def shares(count, total, most, lean, full):
    weights = [(1 << 20) // math.isqrt(standing ** lean) + 1 for standing in range(1, count + 1)]
    largest = most if full else min(most, max(-(-total // count), total * weights[0] // sum(weights)))
    least = 1 if total - largest >= count - 1 else 0
    holding, spare = [largest] + [least] * (count - 1), total - largest - least * (count - 1)
    while spare > 0:
        candidates = [i for i in range(1, count) if holding[i] < largest] or [i for i in range(1, count) if holding[i] < most]
        whole, left = sum([weights[i] for i in candidates]), spare
        for i in candidates:
            addition = min(most - holding[i], max(1, left * weights[i] // whole), spare)
            holding[i] = holding[i] + addition
            spare = spare - addition
    return np.array(holding)


def centred(rng, dims, deviation, reach, cuts=(), held_as=jnp.bfloat16):
    array = jax.random.normal(rng, dims, jnp.float32) * deviation
    if len(cuts) > 0:
        array = block_scale(rng, dims, cuts, -0.22, 0.18) * array
    return jnp.clip(array, min=-reach, max=reach).astype(held_as)


def setup_inputs(seed: int = 0) -> dict:
    seeds = jax.random.split(jax.random.key(seed), 12)
    pooled_in = centred(seeds[0], (TOKENS, D_POOL), 1.0, 6.0, ((0, 8), (1, 4)))
    group_map = centred(seeds[1], (GROUPS, GROUP, GROUP), GROUP ** -0.5, 0.25, ((0, 4),))
    pool_scale = jnp.clip(1.0 + 0.18 * jax.random.normal(seeds[2], (D_POOL,), jnp.float32), 0.1, 1.9)
    out_weight = centred(seeds[3], (D_POOL, D), D_POOL ** -0.5, 0.125, ((0, 4),))
    residual = centred(seeds[4], (TOKENS, D), 1.0, 6.0, ((0, 32),))
    norm_gain = jnp.clip(1.0 + 0.18 * jax.random.normal(seeds[5], (D,), jnp.float32), 0.1, 1.9)
    gate_weight = centred(seeds[6], (EXPERTS, D, FF), D ** -0.5, 0.125, ((0, 8),))
    up_weight = centred(seeds[7], (EXPERTS, D, FF), D ** -0.5, 0.125, ((0, 8),))
    down_weight = centred(seeds[8], (EXPERTS, FF, D), FF ** -0.5, 0.25, ((0, 8),))
    route_expert_keys = jax.random.split(jax.random.fold_in(seeds[9], 1), TOKENS // ROWS_DEV)
    route_expert_turns = jax.random.permutation(jax.random.fold_in(seeds[9], 3), TOKENS // ROWS_DEV)
    route_expert = jax.vmap(lambda own, number: routed_block(jax.random.fold_in(seeds[9], 2), own, number, ROWS_DEV, EXPERTS, TOP, CAP, 2))(route_expert_keys, route_expert_turns).reshape((TOKENS, TOP))
    route_score = jnp.clip(jnp.exp(math.log(1.0) - 2.9957323 * jax.random.uniform(seeds[10], (TOKENS, TOP), jnp.float32) ** block_scale(seeds[10], (TOKENS, TOP), ((0, 32),), -0.2, 0.2)), 0.05, 1.0)
    return dict(pooled_in=pooled_in, group_map=group_map, pool_scale=pool_scale, out_weight=out_weight, residual=residual, norm_gain=norm_gain, gate_weight=gate_weight, up_weight=up_weight, down_weight=down_weight, route_expert=route_expert, route_score=route_score)


def reference(pooled_in, group_map, pool_scale, out_weight, residual, norm_gain, gate_weight, up_weight, down_weight, route_expert, route_score):
    columns = []
    for group_index in range(GROUPS):
        window = 2 ** (group_index + 1)
        channels = pooled_in[:, group_index * GROUP:(group_index + 1) * GROUP].astype(jnp.float32)
        padded = jnp.pad(channels, ((window - 1, 0), (0, 0)))
        running = jnp.zeros_like(channels)
        for offset in range(window):
            running = running + padded[window - 1 - offset:window - 1 - offset + TOKENS]
        counts = jnp.minimum(jnp.arange(TOKENS) + 1, window).astype(jnp.float32)
        contrast = (running / counts[:, None] - channels).astype(jnp.bfloat16)
        mixture = jnp.dot(contrast, group_map[group_index], preferred_element_type=jnp.float32)
        scales = pool_scale[group_index * GROUP:(group_index + 1) * GROUP]
        columns.append((mixture * scales[None, :]).astype(jnp.bfloat16))
    pooled = jnp.concatenate(columns, axis=1)
    projected = jnp.dot(pooled, out_weight, preferred_element_type=jnp.float32)
    middle = (residual.astype(jnp.float32) + projected).astype(jnp.bfloat16)
    middle_f = middle.astype(jnp.float32)
    factor = lax.rsqrt(lax.optimization_barrier(jnp.mean(middle_f * middle_f, axis=1, keepdims=True)) + 1e-06)
    normed = (middle_f * factor * norm_gain[None, :]).astype(jnp.bfloat16)
    share = route_score / lax.optimization_barrier(jnp.sum(route_score, axis=1, keepdims=True))
    blocks = TOKENS // ROWS_DEV
    assigned = route_expert.reshape(blocks, ROWS_DEV * TOP).astype(jnp.int32)
    onehot = (assigned[:, :, None] == jnp.arange(EXPERTS, dtype=jnp.int32)[None, None, :]).astype(jnp.int32)
    slot_rank = lax.optimization_barrier(jnp.sum(jnp.cumsum(onehot, axis=1) * onehot, axis=2)) - 1
    slot_index = (assigned * CAP + slot_rank).astype(jnp.int32)
    token_ids = (jnp.arange(blocks, dtype=jnp.int32)[:, None] * ROWS_DEV + jnp.arange(ROWS_DEV * TOP, dtype=jnp.int32)[None, :] // TOP).astype(jnp.int32)
    block_ids = jnp.broadcast_to(jnp.arange(blocks, dtype=jnp.int32)[:, None], slot_index.shape)
    slot_token = jnp.full((blocks, EXPERTS * CAP), TOKENS, jnp.int32).at[block_ids, slot_index].set(token_ids)
    slot_share = jnp.zeros((blocks, EXPERTS * CAP), jnp.float32).at[block_ids, slot_index].set(share.reshape(blocks, ROWS_DEV * TOP))
    token_by_expert = slot_token.reshape(blocks, EXPERTS, CAP).transpose(1, 0, 2).reshape(EXPERTS, blocks * CAP)
    share_by_expert = slot_share.reshape(blocks, EXPERTS, CAP).transpose(1, 0, 2).reshape(EXPERTS, blocks * CAP)
    padded_rows = jnp.concatenate([normed, jnp.zeros((1, D), jnp.bfloat16)], axis=0)

    def visit(totals, inputs):
        row_ids, row_share, gate_one, up_one, down_one = inputs
        rows_in = padded_rows[row_ids]
        gate_part = jnp.dot(rows_in, gate_one, preferred_element_type=jnp.float32)
        up_part = jnp.dot(rows_in, up_one, preferred_element_type=jnp.float32)
        hidden = (jax.nn.silu(gate_part) * up_part).astype(jnp.bfloat16)
        produced = jnp.dot(hidden, down_one, preferred_element_type=jnp.float32).astype(jnp.bfloat16)
        totals = totals.at[row_ids].add(produced.astype(jnp.float32) * row_share[:, None])
        return (totals, None)
    totals, _ = lax.scan(visit, jnp.zeros((TOKENS + 1, D), jnp.float32), (token_by_expert, share_by_expert, gate_weight, up_weight, down_weight))
    return (middle_f + totals[:TOKENS]).astype(jnp.bfloat16)
```

```python
import jax
import jax.numpy as jnp
from jax import lax
from jax.experimental import pallas as pl
from jax.experimental.pallas import tpu as pltpu
from jax.sharding import PartitionSpec as P


GROUPS = 4
HALO = 16
CHUNKS = 1

f32 = jnp.float32
bf16 = jnp.bfloat16


def dot(a, b):
    return jnp.dot(a, b, preferred_element_type=f32)


def crossed(value, axis, partner):
    peers = lax.axis_size(axis)
    return lax.ppermute(value, axis, [(i, partner(i)) for i in range(peers)])


def pool_kernel(where_ref, halo_ref, x_ref, map_ref, scale_ref, out_ref, ext_ref):
    step = pl.program_id(0)
    rows = out_ref.shape[0]
    window = where_ref[0]
    first = where_ref[1] + step * rows

    @pl.when(step == 0)
    def _():
        ext_ref[0:HALO, :] = halo_ref[...]

    ext_ref[HALO:, :] = x_ref[...]
    behind = (
        lax.broadcasted_iota(jnp.int32, (rows, rows + HALO), 0)
        + HALO
        - lax.broadcasted_iota(jnp.int32, (rows, rows + HALO), 1)
    )
    band = jnp.where((behind >= 0) & (behind < window), 1.0, 0.0).astype(bf16)
    sums = dot(band, ext_ref[...])
    position = first + lax.broadcasted_iota(jnp.int32, (rows, 1), 0)
    counts = jnp.minimum(position + 1, window).astype(f32)
    contrast = (sums / counts - x_ref[...].astype(f32)).astype(bf16)
    out_ref[...] = (dot(contrast, map_ref[0]) * scale_ref[...]).astype(bf16)
    ext_ref[0:HALO, :] = x_ref[rows - HALO :, :]


def pooled_channels(pooled_in, group_map, pool_scale):
    rows, width = pooled_in.shape
    steps = lax.axis_size("tp")
    block = rows // steps
    peers = lax.axis_size("sp")
    halo = lax.ppermute(
        pooled_in[rows - HALO :], "sp", [(i, i + 1) for i in range(peers - 1)]
    )
    window = jnp.left_shift(jnp.int32(2), lax.axis_index("tp"))
    where = jnp.stack([window, lax.axis_index("sp") * rows]).astype(jnp.int32)
    return pl.pallas_call(
        pool_kernel,
        grid=(steps,),
        in_specs=[
            pl.BlockSpec(memory_space=pltpu.SMEM),
            pl.BlockSpec((HALO, width), lambda i: (0, 0)),
            pl.BlockSpec((block, width), lambda i: (i, 0)),
            pl.BlockSpec((1, width, width), lambda i: (0, 0, 0)),
            pl.BlockSpec((1, width), lambda i: (0, 0)),
        ],
        out_specs=pl.BlockSpec((block, width), lambda i: (i, 0)),
        out_shape=jax.ShapeDtypeStruct((rows, width), bf16),
        scratch_shapes=[pltpu.VMEM((block + HALO, width), bf16)],
        name="pool",
    )(where, halo, pooled_in, group_map, pool_scale[None, :])


def reversed_pairs(count):
    return lambda i: (count - 2 - (i // 2) * 2) + i % 2


def body(
    pooled_in,
    group_map,
    pool_scale,
    out_weight,
    residual,
    norm_gain,
    gate_weight,
    up_weight,
    down_weight,
    route_expert,
    route_score,
):
    experts = lax.axis_size("sp")
    replicas = lax.axis_size("tp")
    sp_at = lax.axis_index("sp")
    tp_at = lax.axis_index("tp")
    rows, width = residual.shape
    hidden_units = gate_weight.shape[2]
    top = route_expert.shape[1]
    capacity = max(2, 3 * rows * top // (2 * experts))
    group = experts // 2
    other_half = reversed_pairs(experts)

    part = hidden_units // replicas
    start = tp_at * part
    gate_up = jnp.concatenate(
        [
            lax.dynamic_slice(gate_weight[0], (0, start), (width, part)),
            lax.dynamic_slice(up_weight[0], (0, start), (width, part)),
        ],
        axis=1,
    )
    down = lax.dynamic_slice(down_weight[0], (start, 0), (part, width))
    far_in = [crossed(gate_up, "sp", other_half)]
    far_out = [crossed(down, "sp", other_half)]
    bit = replicas // 2
    while bit:
        far_in = far_in + [crossed(v, "tp", lambda i, b=bit: i ^ b) for v in far_in]
        far_out = far_out + [crossed(v, "tp", lambda i, b=bit: i ^ b) for v in far_out]
        bit //= 2

    mate_weight = crossed(out_weight, "tp", lambda i: i ^ 1)
    pooled = pooled_channels(pooled_in, group_map, pool_scale)
    blocks = pooled.reshape(replicas // 2, 2, rows, -1)
    lane = tp_at % 2
    kept = lax.dynamic_index_in_dim(blocks, lane, 1, keepdims=False)
    given = lax.dynamic_index_in_dim(blocks, 1 - lane, 1, keepdims=False)
    taken = crossed(given, "tp", lambda i: i ^ 1)

    def partial_sums(block_at):
        mine = lax.dynamic_index_in_dim(kept, block_at, 0, keepdims=False)
        mates = lax.dynamic_index_in_dim(taken, block_at, 0, keepdims=False)
        return dot(mine, out_weight) + dot(mates, mate_weight)

    pair_at = tp_at // 2
    projected = residual.astype(f32) + partial_sums(pair_at)
    for hop in range(1, replicas // 2):
        sent = partial_sums(pair_at ^ hop).astype(bf16)
        projected = projected + crossed(sent, "tp", lambda i, h=hop: i ^ (2 * h)).astype(f32)
    middle = projected.astype(bf16)

    here = jnp.arange(experts, dtype=jnp.int32)
    owner = jnp.where(here // group == sp_at // group, here, other_half(here))
    block_of = 2 * (owner ^ sp_at) + (owner != here).astype(jnp.int32)
    named = route_expert[:, :, None] == here[None, None, :]
    hits = jnp.any(named, axis=1)
    earlier = jnp.arange(rows)[:, None] > jnp.arange(rows)[None, :]
    rank = dot(earlier.astype(bf16), hits.astype(bf16)).astype(jnp.int32)
    slot_of = block_of[None, :] * capacity + rank
    slots = jnp.sum(jnp.where(named, slot_of[:, None, :], 0), axis=2)
    shares = route_score / jnp.sum(route_score, axis=1, keepdims=True)
    slot_count = experts * capacity
    picks = slots.T[:, None, :] == jnp.arange(slot_count, dtype=jnp.int32)[None, :, None]
    pick = jnp.any(picks, axis=0).astype(bf16)
    placed = slots[:, :, None] == jnp.arange(slot_count, dtype=jnp.int32)[None, None, :]
    weigh = jnp.sum(jnp.where(placed, shares[:, :, None], 0.0), axis=1)
    weigh_high = weigh.astype(bf16)
    weigh_low = (weigh - weigh_high.astype(f32)).astype(bf16)

    def exchanged(v):
        out = [v[0]]
        for k in range(1, group):
            out.append(crossed(v[k], "sp", lambda i, k=k: i ^ k))
        return jnp.stack(out)

    outgoing = dot(pick, middle).astype(bf16).reshape(group, 2 * capacity, width)
    arrived = exchanged(outgoing).reshape(group, 2, capacity, width)
    returned = []
    for side in range(2):
        lines = arrived[:, side].reshape(group * capacity, width)
        lines_f = lines.astype(f32)
        factor = lax.rsqrt(jnp.mean(lines_f * lines_f, axis=1, keepdims=True) + 1e-06)
        normed = (lines_f * factor * norm_gain[None, :]).astype(bf16)
        if side == 0:
            gate_part = dot(normed, gate_weight[0])
            up_part = dot(normed, up_weight[0])
            hidden = (jax.nn.silu(gate_part) * up_part).astype(bf16)
            produced = dot(hidden, down_weight[0])
        else:
            produced = 0.0
            for w_in, w_out in zip(far_in, far_out):
                both = dot(normed, w_in)
                hidden = (jax.nn.silu(both[:, :part]) * both[:, part:]).astype(bf16)
                produced = produced + dot(hidden, w_out)
        produced = produced.astype(bf16).reshape(group, capacity, width)
        returned.append(exchanged(produced))
    back = jnp.stack(returned, axis=1).reshape(slot_count, width)
    combined = dot(weigh_high, back) + dot(weigh_low, back)
    return (middle.astype(f32) + combined).astype(bf16)


def solution(mesh):
    in_specs = (
        P("sp", "tp"),
        P("tp", None, None),
        P("tp"),
        P("tp", None),
        P(("sp", "tp"), None),
        P(),
        P("sp", None, None),
        P("sp", None, None),
        P("sp", None, None),
        P(("sp", "tp"), None),
        P(("sp", "tp"), None),
    )
    out_specs = P(("sp", "tp"), None)
    return jax.shard_map(body, mesh=mesh, in_specs=in_specs, out_specs=out_specs, check_vma=False)
```

```python
import functools

import jax
import jax.numpy as jnp
from jax import lax
from jax.experimental import pallas as pl
from jax.experimental.pallas import tpu as pltpu
from jax.sharding import PartitionSpec as P


HALO = 16
CHUNKS = 2

f32 = jnp.float32
bf16 = jnp.bfloat16

VMEM = pl.BlockSpec(memory_space=pltpu.VMEM)
SMEM = pl.BlockSpec(memory_space=pltpu.SMEM)
ANY = pl.BlockSpec(memory_space=pl.ANY)


def dot(a, b):
    return jnp.dot(a, b, preferred_element_type=f32)


def crossed(value, axis, partner):
    peers = lax.axis_size(axis)
    return lax.ppermute(value, axis, [(i, partner(i)) for i in range(peers)])


def flipped(value, axis, bits):
    return crossed(value, axis, lambda i: i ^ bits)


def after(value, *others):
    return lax.optimization_barrier((value, *others))[0]


def reversed_pairs(count):
    return lambda i: (count - 2 - (i // 2) * 2) + i % 2


def pool_kernel(at_ref, halo_ref, x_ref, map_ref, scale_ref, *rest):
    out_refs = rest
    blocks = len(out_refs)
    rows = x_ref.shape[0] // blocks
    window = at_ref[0]
    behind = lax.broadcasted_iota(jnp.int32, (rows, rows), 0) - lax.broadcasted_iota(
        jnp.int32, (rows, rows), 1
    )
    band = jnp.where((behind >= 0) & (behind < window), 1.0, 0.0).astype(bf16)
    early = (
        HALO
        + lax.broadcasted_iota(jnp.int32, (HALO, HALO), 0)
        - lax.broadcasted_iota(jnp.int32, (HALO, HALO), 1)
    )
    early_band = jnp.where(early < window, 1.0, 0.0).astype(bf16)
    for k in [*range(1, blocks, 2), *range(0, blocks, 2)]:
        block = at_ref[2] ^ k
        x = x_ref[pl.ds(pl.multiple_of(block * rows, rows), rows), :]
        before = pl.multiple_of(jnp.maximum(block * rows - HALO, 0), HALO)
        tail = jnp.where(block == 0, halo_ref[...], x_ref[pl.ds(before, HALO), :])
        sums = dot(band, x)
        sums = jnp.concatenate([sums[:HALO] + dot(early_band, tail), sums[HALO:]], axis=0)
        position = at_ref[1] + block * rows + lax.broadcasted_iota(jnp.int32, (rows, 1), 0)
        share = 1.0 / jnp.minimum(position + 1, window).astype(f32)
        contrast = (sums * share - x.astype(f32)).astype(bf16)
        out_refs[k][...] = (dot(contrast, map_ref[0]) * scale_ref[...]).astype(bf16)


def pooled_blocks(pooled_in, group_map, pool_scale):
    rows, width = pooled_in.shape
    replicas = lax.axis_size("tp")
    peers = lax.axis_size("sp")
    halo = lax.ppermute(
        pooled_in[rows - HALO :], "sp", [(i, i + 1) for i in range(peers - 1)]
    )
    tp_at = lax.axis_index("tp")
    at = jnp.stack([jnp.left_shift(jnp.int32(2), tp_at), lax.axis_index("sp") * rows, tp_at])
    return pl.pallas_call(
        pool_kernel,
        in_specs=[SMEM, VMEM, VMEM, VMEM, VMEM],
        out_specs=[VMEM] * replicas,
        out_shape=[jax.ShapeDtypeStruct((rows // replicas, width), bf16)] * replicas,
        name="pool",
    )(at.astype(jnp.int32), halo, pooled_in, group_map, pool_scale[None, :])


def project_kernel(count, *refs):
    mine = refs[:count]
    mates = refs[count : 2 * count]
    w_mine, w_mate, residual = refs[2 * count : 2 * count + 3]
    outs = refs[2 * count + 3 : -1]
    lines = refs[-1]
    rows, width = mine[0].shape

    @pl.when(pl.program_id(0) == 0)
    def _():
        for n in range(count):
            lines[n * rows : (n + 1) * rows, :width] = mine[n][...]
            lines[n * rows : (n + 1) * rows, width:] = mates[n][...]

    sums = dot(lines[:, :width], w_mine[...]) + dot(lines[:, width:], w_mate[...])
    outs[0][...] = sums[:rows] + residual[...].astype(f32)
    for n in range(1, count):
        outs[n][...] = sums[n * rows : (n + 1) * rows].astype(bf16)


def projections(mine, mates, w_mine, w_mate, residual, chunk, columns):
    count = len(mine)
    rows, width = mine[0].shape
    step = min(512, columns)
    steps = columns // step
    whole = pl.BlockSpec((rows, width), lambda j: (0, 0))
    weight = pl.BlockSpec((width, step), lambda j: (0, chunk * steps + j))
    tile = pl.BlockSpec((rows, step), lambda j: (0, j))
    return pl.pallas_call(
        functools.partial(project_kernel, count),
        grid=(steps,),
        in_specs=[whole] * (2 * count)
        + [weight, weight, pl.BlockSpec((rows, step), lambda j: (0, chunk * steps + j))],
        out_specs=[tile] * count,
        out_shape=[jax.ShapeDtypeStruct((rows, columns), f32)]
        + [jax.ShapeDtypeStruct((rows, columns), bf16)] * (count - 1),
        scratch_shapes=[pltpu.VMEM((count * rows, 2 * width), bf16)],
        name="project",
    )(*mine, *mates, w_mine, w_mate, residual)


def send_kernel(others, slots_ref, own_ref, *refs):
    parts = refs[:others]
    middle_ref = refs[others]
    outs = refs[others + 1 :]
    total = own_ref[...]
    for part in parts:
        total = total + part[...].astype(f32)
    middle = total.astype(bf16)
    middle_ref[...] = middle
    length = outs[0].shape[0]
    rows = own_ref.shape[0]
    for k, out in enumerate(outs):
        slot = k * length + lax.broadcasted_iota(jnp.int32, (length, rows), 0)
        hit = slot == slots_ref[0:1, :]
        for j in range(1, slots_ref.shape[0]):
            hit = hit | (slot == slots_ref[j : j + 1, :])
        out[...] = dot(jnp.where(hit, 1.0, 0.0).astype(bf16), middle).astype(bf16)


def rows_to_send(slots_t, own, parts, group, length):
    rows, columns = own.shape
    return pl.pallas_call(
        functools.partial(send_kernel, len(parts)),
        in_specs=[VMEM] * (2 + len(parts)),
        out_specs=[VMEM] * (1 + group),
        out_shape=[jax.ShapeDtypeStruct((rows, columns), bf16)]
        + [jax.ShapeDtypeStruct((length, columns), bf16)] * group,
        name="send",
    )(slots_t, own, *parts)


def expert_kernel(group, chunks, swapped, pieces, at_ref, gain_ref, *refs):
    row_refs = refs[: group * chunks]
    refs = refs[group * chunks :]
    weights = refs[: 2 * pieces if swapped else 3]
    refs = refs[len(weights) :]
    outs = refs[:group]
    lines, gate_up, down, sems = refs[group:]
    capacity = outs[0].shape[0]
    part = lines.shape[1] // pieces
    hidden_units = gate_up.shape[3]

    def copies(k):
        if swapped:
            both, out = weights[2 * k], weights[2 * k + 1]
            return (
                pltpu.make_async_copy(both.at[0:part, :], gate_up.at[k, 0], sems.at[k, 0]),
                pltpu.make_async_copy(
                    both.at[part : 2 * part, :], gate_up.at[k, 1], sems.at[k, 1]
                ),
                pltpu.make_async_copy(out, down.at[k], sems.at[k, 2]),
            )
        gate, up, out = weights
        span = pl.ds(k * part, part)
        return (
            pltpu.make_async_copy(gate.at[0, span, :], gate_up.at[k, 0], sems.at[k, 0]),
            pltpu.make_async_copy(up.at[0, span, :], gate_up.at[k, 1], sems.at[k, 1]),
            pltpu.make_async_copy(out.at[0, :, span], down.at[k], sems.at[k, 2]),
        )

    moves = [copies(k) for k in range(pieces)]
    for k in range(pieces):
        moves[k][0].start()
        moves[k][1].start()
    for k in range(pieces):
        moves[k][2].start()
    for p in range(group):
        blocks = [row_refs[p * chunks + c][...].astype(f32) for c in range(chunks)]
        square = sum(jnp.sum(b * b, axis=1, keepdims=True) for b in blocks)
        factor = lax.rsqrt(square / lines.shape[1] + 1e-06)
        at = 0
        for b in blocks:
            span = slice(at, at + b.shape[1])
            lines[p * capacity : (p + 1) * capacity, span] = (
                b * factor * gain_ref[:, span]
            ).astype(bf16)
            at += b.shape[1]

    def offset(k):
        if swapped:
            return pl.multiple_of((at_ref[0] ^ k) * part, part)
        return k * part

    gate_part = jnp.zeros((group * capacity, hidden_units), f32)
    up_part = jnp.zeros((group * capacity, hidden_units), f32)
    for k in range(pieces):
        moves[k][0].wait()
        moves[k][1].wait()
        x = lines[:, pl.ds(offset(k), part)]
        gate_part = gate_part + dot(x, gate_up[k, 0])
        up_part = up_part + dot(x, gate_up[k, 1])
    hidden = (gate_part / (1.0 + jnp.exp(-gate_part)) * up_part).astype(bf16)
    for k in range(pieces):
        moves[k][2].wait()
        made = dot(hidden, down[k]).astype(bf16)
        for p in range(group):
            outs[p][:, pl.ds(offset(k), part)] = made[p * capacity : (p + 1) * capacity]


def expert(row_blocks, side, norm_gain, weights, swapped):
    group = len(row_blocks)
    chunks = len(row_blocks[0])
    capacity = row_blocks[0][0].shape[0] // 2
    pieces = lax.axis_size("tp")
    width = norm_gain.shape[0]
    hidden_units = weights[0].shape[-1]
    part = width // pieces
    flat = [b for blocks in row_blocks for b in blocks]
    return pl.pallas_call(
        functools.partial(expert_kernel, group, chunks, swapped, pieces),
        grid=(1,),
        in_specs=[SMEM, pl.BlockSpec((1, width), lambda i: (0, 0))]
        + [pl.BlockSpec((capacity, b.shape[1]), lambda i: (side, 0)) for b in flat]
        + [ANY] * len(weights),
        out_specs=[pl.BlockSpec((capacity, width), lambda i: (0, 0))] * group,
        out_shape=[jax.ShapeDtypeStruct((capacity, width), bf16)] * group,
        scratch_shapes=[
            pltpu.VMEM((group * capacity, width), bf16),
            pltpu.VMEM((pieces, 2, part, hidden_units), bf16),
            pltpu.VMEM((pieces, hidden_units, part), bf16),
            pltpu.SemaphoreType.DMA((pieces, 3)),
        ],
        name="expert_swapped" if swapped else "expert_own",
    )(lax.axis_index("tp")[None], norm_gain[None, :], *flat, *weights)


def combine_kernel(group, side, slots_ref, share_ref, base_ref, *refs):
    row_refs = refs[:group]
    out_ref, back = refs[group:]
    capacity = row_refs[0].shape[0]
    rows = base_ref.shape[0]
    for p in range(group):
        back[p * capacity : (p + 1) * capacity, :] = row_refs[p][...]
    column = lax.broadcasted_iota(jnp.int32, (rows, group * capacity), 1)
    peer = sum((column >= p * capacity).astype(jnp.int32) for p in range(1, group))
    slot = column + (peer + side) * capacity
    weigh = jnp.zeros((rows, group * capacity), f32)
    for j in range(slots_ref.shape[1]):
        weigh = weigh + jnp.where(slot == slots_ref[:, j : j + 1], share_ref[:, j : j + 1], 0.0)
    high = weigh.astype(bf16)
    low = (weigh - high.astype(f32)).astype(bf16)
    total = base_ref[...].astype(f32) + dot(high, back[...]) + dot(low, back[...])
    out_ref[...] = total.astype(out_ref.dtype)


def combined(slots, shares, base, returned, side, dtype):
    group = len(returned)
    capacity, width = returned[0].shape
    return pl.pallas_call(
        functools.partial(combine_kernel, group, side),
        in_specs=[VMEM] * (3 + group),
        out_specs=VMEM,
        out_shape=jax.ShapeDtypeStruct(base.shape, dtype),
        scratch_shapes=[pltpu.VMEM((group * capacity, width), bf16)],
        name="combine",
    )(slots, shares, base, *returned)


def body(
    pooled_in,
    group_map,
    pool_scale,
    out_weight,
    residual,
    norm_gain,
    gate_weight,
    up_weight,
    down_weight,
    route_expert,
    route_score,
):
    experts = lax.axis_size("sp")
    replicas = lax.axis_size("tp")
    sp_at = lax.axis_index("sp")
    tp_at = lax.axis_index("tp")
    rows, width = residual.shape
    top = route_expert.shape[1]
    capacity = max(2, 3 * rows * top // (2 * experts))
    capacity = -(-capacity // 16) * 16
    group = experts // 2
    other_half = reversed_pairs(experts)
    columns = width // CHUNKS

    part = width // replicas
    start = tp_at * part
    gate_up = jnp.concatenate(
        [
            lax.dynamic_slice_in_dim(gate_weight[0], start, part, 0),
            lax.dynamic_slice_in_dim(up_weight[0], start, part, 0),
        ],
        axis=0,
    )
    down = lax.dynamic_slice_in_dim(down_weight[0], start, part, 1)
    far = [(0, crossed(gate_up, "sp", other_half), crossed(down, "sp", other_half))]

    here = jnp.arange(experts, dtype=jnp.int32)
    owner = jnp.where(here // group == sp_at // group, here, other_half(here))
    block_of = 2 * (owner ^ sp_at) + (owner != here).astype(jnp.int32)
    named = route_expert[:, :, None] == here[None, None, :]
    hits = jnp.any(named, axis=1)
    earlier = jnp.arange(rows)[:, None] > jnp.arange(rows)[None, :]
    rank = dot(earlier.astype(bf16), hits.astype(bf16)).astype(jnp.int32)
    slot_of = block_of[None, :] * capacity + rank
    slots = jnp.sum(jnp.where(named, slot_of[:, None, :], 0), axis=2)
    slots_t = slots.T
    shares = route_score / jnp.sum(route_score, axis=1, keepdims=True)

    mate_weight = flipped(out_weight, "tp", 1)
    pooled = pooled_blocks(pooled_in, group_map, pool_scale)
    mine = pooled[0::2]
    mates = [flipped(v, "tp", 1) for v in pooled[1::2]]
    sums = [
        projections(mine, mates, out_weight, mate_weight, residual, c, columns)
        for c in range(CHUNKS)
    ]
    middles = []
    arrived = [[] for _ in range(group)]
    for c in range(CHUNKS):
        own, *leaving = sums[c]
        parts = [flipped(v, "tp", 2 * (n + 1)) for n, v in enumerate(leaving)]
        middle, *outgoing = rows_to_send(slots_t, own, parts, group, 2 * capacity)
        middles.append(middle)
        arrived[0].append(outgoing[0])
        for k in range(1, group):
            arrived[k].append(flipped(outgoing[k], "sp", k))
    middle = jnp.concatenate(middles, axis=1)

    bit = replicas // 2
    far = [(k, after(v, *outgoing), after(w, *outgoing)) for k, v, w in far]
    while bit:
        far = far + [
            (k ^ bit, flipped(v, "tp", bit), flipped(w, "tp", bit)) for k, v, w in far
        ]
        bit //= 2
    far.sort(key=lambda entry: entry[0])
    far_weights = [v for entry in far for v in entry[1:]]

    def sent_back(made):
        return [made[0]] + [flipped(made[k], "sp", k) for k in range(1, group)]

    made = expert(arrived, 0, norm_gain, (gate_weight, up_weight, down_weight), False)
    back = sent_back(made)
    made = expert(arrived, 1, norm_gain, far_weights, True)
    far_back = sent_back(made)
    total = combined(slots, shares, middle, back, 0, f32)
    return combined(slots, shares, total, far_back, 1, bf16)


def solution(mesh):
    in_specs = (
        P("sp", "tp"),
        P("tp", None, None),
        P("tp"),
        P("tp", None),
        P(("sp", "tp"), None),
        P(),
        P("sp", None, None),
        P("sp", None, None),
        P("sp", None, None),
        P(("sp", "tp"), None),
        P(("sp", "tp"), None),
    )
    out_specs = P(("sp", "tp"), None)
    return jax.shard_map(body, mesh=mesh, in_specs=in_specs, out_specs=out_specs, check_vma=False)
```

```python
import functools

import jax
import jax.numpy as jnp
from jax import lax
from jax.experimental import pallas as pl
from jax.experimental.pallas import tpu as pltpu
from jax.sharding import PartitionSpec as P


HALO = 16
CHUNKS = 2

f32 = jnp.float32
bf16 = jnp.bfloat16

VMEM = pl.BlockSpec(memory_space=pltpu.VMEM)
SMEM = pl.BlockSpec(memory_space=pltpu.SMEM)
ANY = pl.BlockSpec(memory_space=pl.ANY)


def dot(a, b):
    return jnp.dot(a, b, preferred_element_type=f32)


def crossed(value, axis, partner):
    peers = lax.axis_size(axis)
    return lax.ppermute(value, axis, [(i, partner(i)) for i in range(peers)])


def flipped(value, axis, bits):
    return crossed(value, axis, lambda i: i ^ bits)


def reversed_pairs(count):
    return lambda i: (count - 2 - (i // 2) * 2) + i % 2


def pool_kernel(at_ref, halo_ref, x_ref, map_ref, scale_ref, *rest):
    out_refs = rest
    blocks = len(out_refs)
    rows = x_ref.shape[0] // blocks
    window = at_ref[0]
    behind = lax.broadcasted_iota(jnp.int32, (rows, rows), 0) - lax.broadcasted_iota(
        jnp.int32, (rows, rows), 1
    )
    band = jnp.where((behind >= 0) & (behind < window), 1.0, 0.0).astype(bf16)
    early = (
        HALO
        + lax.broadcasted_iota(jnp.int32, (HALO, HALO), 0)
        - lax.broadcasted_iota(jnp.int32, (HALO, HALO), 1)
    )
    early_band = jnp.where(early < window, 1.0, 0.0).astype(bf16)
    for k in [*range(1, blocks, 2), *range(0, blocks, 2)]:
        block = at_ref[2] ^ k
        x = x_ref[pl.ds(pl.multiple_of(block * rows, rows), rows), :]
        before = pl.multiple_of(jnp.maximum(block * rows - HALO, 0), HALO)
        tail = jnp.where(block == 0, halo_ref[...], x_ref[pl.ds(before, HALO), :])
        sums = dot(band, x)
        sums = jnp.concatenate([sums[:HALO] + dot(early_band, tail), sums[HALO:]], axis=0)
        position = at_ref[1] + block * rows + lax.broadcasted_iota(jnp.int32, (rows, 1), 0)
        share = 1.0 / jnp.minimum(position + 1, window).astype(f32)
        contrast = (sums * share - x.astype(f32)).astype(bf16)
        out_refs[k][...] = (dot(contrast, map_ref[0]) * scale_ref[...]).astype(bf16)


def pooled_blocks(pooled_in, group_map, pool_scale):
    rows, width = pooled_in.shape
    replicas = lax.axis_size("tp")
    peers = lax.axis_size("sp")
    halo = lax.ppermute(
        pooled_in[rows - HALO :], "sp", [(i, i + 1) for i in range(peers - 1)]
    )
    tp_at = lax.axis_index("tp")
    at = jnp.stack([jnp.left_shift(jnp.int32(2), tp_at), lax.axis_index("sp") * rows, tp_at])
    return pl.pallas_call(
        pool_kernel,
        in_specs=[SMEM, VMEM, VMEM, VMEM, VMEM],
        out_specs=[VMEM] * replicas,
        out_shape=[jax.ShapeDtypeStruct((rows // replicas, width), bf16)] * replicas,
        name="pool",
    )(at.astype(jnp.int32), halo, pooled_in, group_map, pool_scale[None, :])


def project_kernel(count, *refs):
    mine = refs[:count]
    mates = refs[count : 2 * count]
    w_mine, w_mate, residual = refs[2 * count : 2 * count + 3]
    outs = refs[2 * count + 3 : -1]
    lines = refs[-1]
    rows, width = mine[0].shape

    @pl.when(pl.program_id(0) == 0)
    def _():
        for n in range(count):
            lines[n * rows : (n + 1) * rows, :width] = mine[n][...]
            lines[n * rows : (n + 1) * rows, width:] = mates[n][...]

    sums = dot(lines[:, :width], w_mine[...]) + dot(lines[:, width:], w_mate[...])
    outs[0][...] = sums[:rows] + residual[...].astype(f32)
    for n in range(1, count):
        outs[n][...] = sums[n * rows : (n + 1) * rows].astype(bf16)


def projections(mine, mates, w_mine, w_mate, residual, chunk, columns):
    count = len(mine)
    rows, width = mine[0].shape
    step = min(512, columns)
    steps = columns // step
    whole = pl.BlockSpec((rows, width), lambda j: (0, 0))
    weight = pl.BlockSpec((width, step), lambda j: (0, chunk * steps + j))
    tile = pl.BlockSpec((rows, step), lambda j: (0, j))
    return pl.pallas_call(
        functools.partial(project_kernel, count),
        grid=(steps,),
        in_specs=[whole] * (2 * count)
        + [weight, weight, pl.BlockSpec((rows, step), lambda j: (0, chunk * steps + j))],
        out_specs=[tile] * count,
        out_shape=[jax.ShapeDtypeStruct((rows, columns), f32)]
        + [jax.ShapeDtypeStruct((rows, columns), bf16)] * (count - 1),
        scratch_shapes=[pltpu.VMEM((count * rows, 2 * width), bf16)],
        name="project",
    )(*mine, *mates, w_mine, w_mate, residual)


def send_kernel(others, slots_ref, own_ref, *refs):
    parts = refs[:others]
    middle_ref = refs[others]
    outs = refs[others + 1 :]
    total = own_ref[...]
    for part in parts:
        total = total + part[...].astype(f32)
    middle = total.astype(bf16)
    middle_ref[...] = middle
    length = outs[0].shape[0]
    rows = own_ref.shape[0]
    for k, out in enumerate(outs):
        slot = k * length + lax.broadcasted_iota(jnp.int32, (length, rows), 0)
        hit = slot == slots_ref[0:1, :]
        for j in range(1, slots_ref.shape[0]):
            hit = hit | (slot == slots_ref[j : j + 1, :])
        out[...] = dot(jnp.where(hit, 1.0, 0.0).astype(bf16), middle).astype(bf16)


def rows_to_send(slots_t, own, parts, group, length):
    rows, columns = own.shape
    return pl.pallas_call(
        functools.partial(send_kernel, len(parts)),
        in_specs=[VMEM] * (2 + len(parts)),
        out_specs=[VMEM] * (1 + group),
        out_shape=[jax.ShapeDtypeStruct((rows, columns), bf16)]
        + [jax.ShapeDtypeStruct((length, columns), bf16)] * group,
        name="send",
    )(slots_t, own, *parts)


def expert_kernel(group, chunks, swapped, pieces, at_ref, gain_ref, *refs):
    row_refs = refs[: group * chunks]
    refs = refs[group * chunks :]
    weights = refs[: 2 * pieces if swapped else 3]
    refs = refs[len(weights) :]
    outs = refs[:group]
    lines, gate_up, down, sems = refs[group:]
    capacity = outs[0].shape[0]
    part = lines.shape[1] // pieces
    hidden_units = gate_up.shape[3]

    def copies(k):
        if swapped:
            both, out = weights[2 * k], weights[2 * k + 1]
            return (
                pltpu.make_async_copy(both.at[0:part, :], gate_up.at[k, 0], sems.at[k, 0]),
                pltpu.make_async_copy(
                    both.at[part : 2 * part, :], gate_up.at[k, 1], sems.at[k, 1]
                ),
                pltpu.make_async_copy(out, down.at[k], sems.at[k, 2]),
            )
        gate, up, out = weights
        span = pl.ds(k * part, part)
        return (
            pltpu.make_async_copy(gate.at[0, span, :], gate_up.at[k, 0], sems.at[k, 0]),
            pltpu.make_async_copy(up.at[0, span, :], gate_up.at[k, 1], sems.at[k, 1]),
            pltpu.make_async_copy(out.at[0, :, span], down.at[k], sems.at[k, 2]),
        )

    moves = [copies(k) for k in range(pieces)]
    for k in range(pieces):
        moves[k][0].start()
        moves[k][1].start()
    for k in range(pieces):
        moves[k][2].start()
    for p in range(group):
        blocks = [row_refs[p * chunks + c][...].astype(f32) for c in range(chunks)]
        square = sum(jnp.sum(b * b, axis=1, keepdims=True) for b in blocks)
        factor = lax.rsqrt(square / lines.shape[1] + 1e-06)
        at = 0
        for b in blocks:
            span = slice(at, at + b.shape[1])
            lines[p * capacity : (p + 1) * capacity, span] = (
                b * factor * gain_ref[:, span]
            ).astype(bf16)
            at += b.shape[1]

    def offset(k):
        if swapped:
            return pl.multiple_of((at_ref[0] ^ k) * part, part)
        return k * part

    gate_part = jnp.zeros((group * capacity, hidden_units), f32)
    up_part = jnp.zeros((group * capacity, hidden_units), f32)
    for k in range(pieces):
        moves[k][0].wait()
        moves[k][1].wait()
        x = lines[:, pl.ds(offset(k), part)]
        gate_part = gate_part + dot(x, gate_up[k, 0])
        up_part = up_part + dot(x, gate_up[k, 1])
    hidden = (gate_part / (1.0 + jnp.exp(-gate_part)) * up_part).astype(bf16)
    for k in range(pieces):
        moves[k][2].wait()
        made = dot(hidden, down[k]).astype(bf16)
        for p in range(group):
            outs[p][:, pl.ds(offset(k), part)] = made[p * capacity : (p + 1) * capacity]


def expert(row_blocks, side, norm_gain, weights, swapped):
    group = len(row_blocks)
    chunks = len(row_blocks[0])
    capacity = row_blocks[0][0].shape[0] // 2
    pieces = lax.axis_size("tp")
    width = norm_gain.shape[0]
    hidden_units = weights[0].shape[-1]
    part = width // pieces
    flat = [b for blocks in row_blocks for b in blocks]
    return pl.pallas_call(
        functools.partial(expert_kernel, group, chunks, swapped, pieces),
        grid=(1,),
        in_specs=[SMEM, pl.BlockSpec((1, width), lambda i: (0, 0))]
        + [pl.BlockSpec((capacity, b.shape[1]), lambda i: (side, 0)) for b in flat]
        + [ANY] * len(weights),
        out_specs=[pl.BlockSpec((capacity, width), lambda i: (0, 0))] * group,
        out_shape=[jax.ShapeDtypeStruct((capacity, width), bf16)] * group,
        scratch_shapes=[
            pltpu.VMEM((group * capacity, width), bf16),
            pltpu.VMEM((pieces, 2, part, hidden_units), bf16),
            pltpu.VMEM((pieces, hidden_units, part), bf16),
            pltpu.SemaphoreType.DMA((pieces, 3)),
        ],
        name="expert_swapped" if swapped else "expert_own",
    )(lax.axis_index("tp")[None], norm_gain[None, :], *flat, *weights)


def combine_kernel(group, side, slots_ref, share_ref, *refs):
    row_refs = refs[:group]
    base_refs = refs[group:-2]
    out_ref, back = refs[-2:]
    capacity = row_refs[0].shape[0]
    rows = out_ref.shape[0]
    for p in range(group):
        back[p * capacity : (p + 1) * capacity, :] = row_refs[p][...]
    column = lax.broadcasted_iota(jnp.int32, (rows, group * capacity), 1)
    peer = sum((column >= p * capacity).astype(jnp.int32) for p in range(1, group))
    slot = column + (peer + side) * capacity
    weigh = jnp.zeros((rows, group * capacity), f32)
    for j in range(slots_ref.shape[1]):
        weigh = weigh + jnp.where(slot == slots_ref[:, j : j + 1], share_ref[:, j : j + 1], 0.0)
    high = weigh.astype(bf16)
    low = (weigh - high.astype(f32)).astype(bf16)
    at = 0
    for base in base_refs:
        span = slice(at, at + base.shape[1])
        total = base[...].astype(f32) + dot(high, back[:, span]) + dot(low, back[:, span])
        out_ref[:, span] = total.astype(out_ref.dtype)
        at += base.shape[1]


def combined(slots, shares, bases, returned, side, dtype):
    group = len(returned)
    capacity, width = returned[0].shape
    steps = 4 if len(bases) == 1 else 1
    tile = lambda v: pl.BlockSpec((v.shape[0], v.shape[1] // steps), lambda j: (0, j))
    small = pl.BlockSpec(slots.shape, lambda j: (0, 0))
    out = jax.ShapeDtypeStruct((slots.shape[0], width), dtype)
    return pl.pallas_call(
        functools.partial(combine_kernel, group, side),
        grid=(steps,),
        in_specs=[small, small] + [tile(v) for v in [*returned, *bases]],
        out_specs=tile(out),
        out_shape=out,
        scratch_shapes=[pltpu.VMEM((group * capacity, width // steps), bf16)],
        name="combine",
    )(slots, shares, *returned, *bases)


def body(
    pooled_in,
    group_map,
    pool_scale,
    out_weight,
    residual,
    norm_gain,
    gate_weight,
    up_weight,
    down_weight,
    route_expert,
    route_score,
):
    experts = lax.axis_size("sp")
    replicas = lax.axis_size("tp")
    sp_at = lax.axis_index("sp")
    tp_at = lax.axis_index("tp")
    rows, width = residual.shape
    top = route_expert.shape[1]
    capacity = max(2, 3 * rows * top // (2 * experts))
    capacity = -(-capacity // 16) * 16
    group = experts // 2
    other_half = reversed_pairs(experts)
    columns = width // CHUNKS

    part = width // replicas
    start = tp_at * part
    gate_up = jnp.concatenate(
        [
            lax.dynamic_slice_in_dim(gate_weight[0], start, part, 0),
            lax.dynamic_slice_in_dim(up_weight[0], start, part, 0),
        ],
        axis=0,
    )
    down = lax.dynamic_slice_in_dim(down_weight[0], start, part, 1)
    far = [(0, crossed(gate_up, "sp", other_half), crossed(down, "sp", other_half))]

    here = jnp.arange(experts, dtype=jnp.int32)
    owner = jnp.where(here // group == sp_at // group, here, other_half(here))
    block_of = 2 * (owner ^ sp_at) + (owner != here).astype(jnp.int32)
    named = route_expert[:, :, None] == here[None, None, :]
    hits = jnp.any(named, axis=1)
    earlier = jnp.arange(rows)[:, None] > jnp.arange(rows)[None, :]
    rank = dot(earlier.astype(bf16), hits.astype(bf16)).astype(jnp.int32)
    slot_of = block_of[None, :] * capacity + rank
    slots = jnp.sum(jnp.where(named, slot_of[:, None, :], 0), axis=2)
    slots_t = slots.T
    shares = route_score / jnp.sum(route_score, axis=1, keepdims=True)

    mate_weight = flipped(out_weight, "tp", 1)
    pooled = pooled_blocks(pooled_in, group_map, pool_scale)
    mine = pooled[0::2]
    mates = [flipped(v, "tp", 1) for v in pooled[1::2]]
    sums = []
    for c in range(CHUNKS):
        sums.append(projections(mine, mates, out_weight, mate_weight, residual, c, columns))
    middles = []
    arrived = [[] for _ in range(group)]
    for c in range(CHUNKS):
        own, *leaving = sums[c]
        parts = [flipped(v, "tp", 2 * (n + 1)) for n, v in enumerate(leaving)]
        middle, *outgoing = rows_to_send(slots_t, own, parts, group, 2 * capacity)
        middles.append(middle)
        arrived[0].append(outgoing[0])
        for k in range(1, group):
            arrived[k].append(flipped(outgoing[k], "sp", k))
    bit = replicas // 2
    while bit:
        far = far + [
            (k ^ bit, flipped(v, "tp", bit), flipped(w, "tp", bit))
            for k, v, w in far
        ]
        bit //= 2
    far.sort(key=lambda entry: entry[0])
    far_weights = [v for entry in far for v in entry[1:]]

    def sent_back(made):
        return [made[0]] + [flipped(made[k], "sp", k) for k in range(1, group)]

    made = expert(arrived, 0, norm_gain, (gate_weight, up_weight, down_weight), False)
    back = sent_back(made)
    made = expert(arrived, 1, norm_gain, far_weights, True)
    far_back = sent_back(made)
    total = combined(slots, shares, middles, back, 0, f32)
    return combined(slots, shares, [total], far_back, 1, bf16)


def solution(mesh):
    in_specs = (
        P("sp", "tp"),
        P("tp", None, None),
        P("tp"),
        P("tp", None),
        P(("sp", "tp"), None),
        P(),
        P("sp", None, None),
        P("sp", None, None),
        P("sp", None, None),
        P(("sp", "tp"), None),
        P(("sp", "tp"), None),
    )
    out_specs = P(("sp", "tp"), None)
    return jax.shard_map(body, mesh=mesh, in_specs=in_specs, out_specs=out_specs, check_vma=False)
```

```python
import functools

import jax
import jax.numpy as jnp
from jax import lax
from jax.experimental import pallas as pl
from jax.experimental.pallas import tpu as pltpu
from jax.sharding import PartitionSpec as P


HALO = 16
CHUNKS = 2

f32 = jnp.float32
bf16 = jnp.bfloat16

VMEM = pl.BlockSpec(memory_space=pltpu.VMEM)
SMEM = pl.BlockSpec(memory_space=pltpu.SMEM)
ANY = pl.BlockSpec(memory_space=pl.ANY)


def dot(a, b):
    return jnp.dot(a, b, preferred_element_type=f32)


def flipped(value, axis, bits):
    return lax.ppermute(value, axis, [(i, i ^ bits) for i in range(lax.axis_size(axis))])


def reversed_pairs(count):
    return lambda i: (count - 2 - (i // 2) * 2) + i % 2


def cut_kernel(x_ref, gate_ref, up_ref, down_ref, tail_ref, *rest):
    gate_out, up_out, down_out, sems = rest
    part = down_out.shape[1]
    span = pl.ds(pl.multiple_of(lax.axis_index("tp") * part, part), part)
    rows = x_ref.shape[0]
    moves = [
        pltpu.make_async_copy(source, target, sems.at[n])
        for n, (source, target) in enumerate(
            [
                (x_ref.at[rows - HALO : rows, :], tail_ref),
                (gate_ref.at[0, span, :], gate_out),
                (up_ref.at[0, span, :], up_out),
                (down_ref.at[0, :, span], down_out),
            ]
        )
    ]
    for move in moves:
        move.start()
    for move in moves:
        move.wait()


def cut_out(pooled_in, gate_weight, up_weight, down_weight):
    part = gate_weight.shape[1] // lax.axis_size("tp")
    hidden_units = gate_weight.shape[2]
    return pl.pallas_call(
        cut_kernel,
        in_specs=[ANY] * 4,
        out_specs=[VMEM] * 4,
        out_shape=[
            jax.ShapeDtypeStruct((HALO, pooled_in.shape[1]), bf16),
            jax.ShapeDtypeStruct((part, hidden_units), bf16),
            jax.ShapeDtypeStruct((part, hidden_units), bf16),
            jax.ShapeDtypeStruct((hidden_units, part), bf16),
        ],
        scratch_shapes=[pltpu.SemaphoreType.DMA((4,))],
        name="cut",
    )(pooled_in, gate_weight, up_weight, down_weight)


def pool_kernel(halo_ref, x_ref, map_ref, scale_ref, *rest):
    *kept_refs, given_ref = rest
    blocks = 2 * len(kept_refs)
    rows = x_ref.shape[0] // blocks
    tp_at = lax.axis_index("tp")
    first = lax.axis_index("sp") * x_ref.shape[0]
    window = jnp.left_shift(jnp.int32(2), tp_at)
    behind = lax.broadcasted_iota(jnp.int32, (rows, rows), 0) - lax.broadcasted_iota(
        jnp.int32, (rows, rows), 1
    )
    band = jnp.where((behind >= 0) & (behind < window), 1.0, 0.0).astype(bf16)
    early = (
        HALO
        + lax.broadcasted_iota(jnp.int32, (HALO, HALO), 0)
        - lax.broadcasted_iota(jnp.int32, (HALO, HALO), 1)
    )
    early_band = jnp.where(early < window, 1.0, 0.0).astype(bf16)
    for k in [*range(1, blocks, 2), *range(0, blocks, 2)]:
        block = tp_at ^ k
        x = x_ref[pl.ds(pl.multiple_of(block * rows, rows), rows), :]
        before = pl.multiple_of(jnp.maximum(block * rows - HALO, 0), HALO)
        tail = jnp.where(block == 0, halo_ref[...], x_ref[pl.ds(before, HALO), :])
        sums = dot(band, x)
        sums = jnp.concatenate([sums[:HALO] + dot(early_band, tail), sums[HALO:]], axis=0)
        position = first + block * rows + lax.broadcasted_iota(jnp.int32, (rows, 1), 0)
        share = 1.0 / jnp.minimum(position + 1, window).astype(f32)
        contrast = (sums * share - x.astype(f32)).astype(bf16)
        pooled = (dot(contrast, map_ref[0]) * scale_ref[...]).astype(bf16)
        if k % 2:
            given_ref[k // 2 * rows : (k // 2 + 1) * rows, :] = pooled
        else:
            kept_refs[k // 2][...] = pooled


def pooled_blocks(tail, pooled_in, group_map, pool_scale):
    rows, width = pooled_in.shape
    replicas = lax.axis_size("tp")
    peers = lax.axis_size("sp")
    halo = lax.ppermute(tail, "sp", [(i, i + 1) for i in range(peers - 1)])
    return pl.pallas_call(
        pool_kernel,
        in_specs=[VMEM] * 4,
        out_specs=[VMEM] * (replicas // 2 + 1),
        out_shape=[jax.ShapeDtypeStruct((rows // replicas, width), bf16)] * (replicas // 2)
        + [jax.ShapeDtypeStruct((rows // 2, width), bf16)],
        name="pool",
        compiler_params=pltpu.CompilerParams(vmem_limit_bytes=12 << 20),
    )(halo, pooled_in, group_map, pool_scale[None, :])


def project_kernel(count, *refs):
    mine = refs[:count]
    mates = refs[count : 2 * count]
    w_mine, w_mate = refs[2 * count : 2 * count + 2]
    outs = refs[-count - 1 : -1]
    residual = refs[2 * count + 2 : -count - 1]
    lines = refs[-1]
    rows, width = mine[0].shape

    @pl.when(pl.program_id(0) == 0)
    def _():
        for n in range(count):
            lines[n * rows : (n + 1) * rows, :width] = mine[n][...]
            lines[n * rows : (n + 1) * rows, width:] = mates[n][...]

    sums = dot(lines[:, :width], w_mine[...]) + dot(lines[:, width:], w_mate[...])
    for n in range(count):
        part = sums[n * rows : (n + 1) * rows]
        if residual:
            part = part + residual[0][...].astype(f32)
        outs[n][...] = part.astype(outs[n].dtype)


def projections(mine, mates, first, w_mine, w_mate, residual, chunk, columns):
    count = len(mine)
    rows, width = mine[0].shape
    step = min(512, columns)
    steps = columns // step
    whole = pl.BlockSpec((rows, width), lambda j: (0, 0))
    weight = pl.BlockSpec((width, step), lambda j: (0, chunk * steps + j))
    tile = pl.BlockSpec((rows, step), lambda j: (0, j))
    dtype = f32 if residual else bf16
    return pl.pallas_call(
        functools.partial(project_kernel, count),
        grid=(steps,),
        in_specs=[whole] * count
        + [pl.BlockSpec((rows, width), lambda j, n=n: (first + n, 0)) for n in range(count)]
        + [weight, weight]
        + [pl.BlockSpec((rows, step), lambda j: (0, chunk * steps + j))] * len(residual),
        out_specs=[tile] * count,
        out_shape=[jax.ShapeDtypeStruct((rows, columns), dtype)] * count,
        scratch_shapes=[pltpu.VMEM((count * rows, 2 * width), bf16)],
        name="project",
        compiler_params=pltpu.CompilerParams(vmem_limit_bytes=16 << 20),
    )(*mine, *([mates] * count), w_mine, w_mate, *residual)


def send_kernel(others, slots_ref, own_ref, *refs):
    parts = refs[:others]
    middle_ref, *outs = refs[others:]
    total = own_ref[...]
    for part in parts:
        total = total + part[...].astype(f32)
    middle = total.astype(bf16)
    middle_ref[...] = middle
    length = outs[0].shape[0]
    rows = own_ref.shape[0]
    for k, out in enumerate(outs):
        slot = k * length + lax.broadcasted_iota(jnp.int32, (length, rows), 0)
        hit = slot == slots_ref[0:1, :]
        for j in range(1, slots_ref.shape[0]):
            hit = hit | (slot == slots_ref[j : j + 1, :])
        out[...] = dot(jnp.where(hit, 1.0, 0.0).astype(bf16), middle).astype(bf16)


def rows_to_send(slots_t, own, parts, group, length):
    rows, columns = own.shape
    return pl.pallas_call(
        functools.partial(send_kernel, len(parts)),
        in_specs=[VMEM] * (2 + len(parts)),
        out_specs=[VMEM] * (1 + group),
        out_shape=[jax.ShapeDtypeStruct((rows, columns), bf16)]
        + [jax.ShapeDtypeStruct((length, columns), bf16)] * group,
        name="send",
        compiler_params=pltpu.CompilerParams(vmem_limit_bytes=12 << 20),
    )(slots_t, own, *parts)


def expert_kernel(group, chunks, side, pieces, gain_ref, *refs):
    row_refs = refs[: group * chunks]
    weights = refs[group * chunks : -group - 1]
    outs = refs[-group - 1 : -1]
    lines = refs[-1]
    capacity = outs[0].shape[0]
    part = lines.shape[1] // pieces
    hidden_units = weights[0].shape[-1]
    swapped = len(weights) > 3
    tp_at = lax.axis_index("tp")
    mine = slice(side * capacity, (side + 1) * capacity)
    for p in range(group):
        blocks = [
            (ref[mine, :] if ref.shape[0] > capacity else ref[...]).astype(f32)
            for ref in row_refs[p * chunks : (p + 1) * chunks]
        ]
        square = sum(jnp.sum(b * b, axis=1, keepdims=True) for b in blocks)
        factor = lax.rsqrt(square / lines.shape[1] + 1e-06)
        at = 0
        for b in blocks:
            span = slice(at, at + b.shape[1])
            lines[p * capacity : (p + 1) * capacity, span] = (
                b * factor * gain_ref[:, span]
            ).astype(bf16)
            at += b.shape[1]

    def piece(k):
        if swapped:
            span = pl.ds(pl.multiple_of((tp_at ^ k) * part, part), part)
            gate, up, down = (ref[...] for ref in weights[3 * k : 3 * k + 3])
        else:
            span = slice(k * part, (k + 1) * part)
            gate, up, down = weights[0][0, span, :], weights[1][0, span, :], weights[2][0, :, span]
        return span, gate, up, down

    gate_part = jnp.zeros((group * capacity, hidden_units), f32)
    up_part = jnp.zeros((group * capacity, hidden_units), f32)
    for k in range(pieces):
        span, gate, up, _ = piece(k)
        x = lines[:, span]
        gate_part = gate_part + dot(x, gate)
        up_part = up_part + dot(x, up)
    hidden = (gate_part / (1.0 + jnp.exp(-gate_part)) * up_part).astype(bf16)
    for k in range(pieces):
        span, _, _, down = piece(k)
        made = dot(hidden, down).astype(bf16)
        for p in range(group):
            outs[p][:, span] = made[p * capacity : (p + 1) * capacity]


def expert(row_blocks, side, capacity, norm_gain, weights):
    group = len(row_blocks)
    chunks = len(row_blocks[0])
    width = norm_gain.shape[0]
    flat = [b for blocks in row_blocks for b in blocks]
    return pl.pallas_call(
        functools.partial(expert_kernel, group, chunks, side, lax.axis_size("tp")),
        in_specs=[VMEM] * (1 + len(flat) + len(weights)),
        out_specs=[VMEM] * group,
        out_shape=[jax.ShapeDtypeStruct((capacity, width), bf16)] * group,
        scratch_shapes=[pltpu.VMEM((group * capacity, width), bf16)],
        name="expert_far" if side else "expert_own",
        compiler_params=pltpu.CompilerParams(vmem_limit_bytes=28 << 20),
    )(norm_gain[None, :], *flat, *weights)


def combine_kernel(group, side, slots_ref, share_ref, *refs):
    row_refs = refs[:group]
    base_refs = refs[group:-2]
    out_ref, back = refs[-2:]
    capacity = row_refs[0].shape[0]
    rows = out_ref.shape[0]
    for p in range(group):
        back[p * capacity : (p + 1) * capacity, :] = row_refs[p][...]
    column = lax.broadcasted_iota(jnp.int32, (rows, group * capacity), 1)
    peer = sum((column >= p * capacity).astype(jnp.int32) for p in range(1, group))
    slot = column + (peer + side) * capacity
    weigh = jnp.zeros((rows, group * capacity), f32)
    for j in range(slots_ref.shape[1]):
        weigh = weigh + jnp.where(slot == slots_ref[:, j : j + 1], share_ref[:, j : j + 1], 0.0)
    high = weigh.astype(bf16)
    low = (weigh - high.astype(f32)).astype(bf16)
    at = 0
    for base in base_refs:
        span = slice(at, at + base.shape[1])
        total = base[...].astype(f32) + dot(high, back[:, span]) + dot(low, back[:, span])
        out_ref[:, span] = total.astype(out_ref.dtype)
        at += base.shape[1]


def combined(slots, shares, bases, returned, side, dtype):
    group = len(returned)
    capacity, width = returned[0].shape
    steps = 1
    tile = lambda v: pl.BlockSpec((v.shape[0], v.shape[1] // steps), lambda j: (0, j))
    small = pl.BlockSpec(slots.shape, lambda j: (0, 0))
    out = jax.ShapeDtypeStruct((slots.shape[0], width), dtype)
    return pl.pallas_call(
        functools.partial(combine_kernel, group, side),
        grid=(steps,),
        in_specs=[small, small] + [tile(v) for v in [*returned, *bases]],
        out_specs=tile(out),
        out_shape=out,
        scratch_shapes=[pltpu.VMEM((group * capacity, width // steps), bf16)],
        name="combine",
        compiler_params=pltpu.CompilerParams(vmem_limit_bytes=16 << 20),
    )(slots, shares, *returned, *bases)


def body(
    pooled_in,
    group_map,
    pool_scale,
    out_weight,
    residual,
    norm_gain,
    gate_weight,
    up_weight,
    down_weight,
    route_expert,
    route_score,
):
    experts = lax.axis_size("sp")
    replicas = lax.axis_size("tp")
    sp_at = lax.axis_index("sp")
    rows, width = residual.shape
    top = route_expert.shape[1]
    capacity = max(2, 3 * rows * top // (2 * experts))
    capacity = -(-capacity // 16) * 16
    group = experts // 2
    other_half = reversed_pairs(experts)
    columns = width // CHUNKS

    mate_weight = flipped(out_weight, "tp", 1)
    tail, *pieces = cut_out(pooled_in, gate_weight, up_weight, down_weight)
    pairs = [(i, other_half(i)) for i in range(experts)]
    copied = {0: [lax.ppermute(v, "sp", pairs) for v in pieces]}

    here = jnp.arange(experts, dtype=jnp.int32)
    owner = jnp.where(here // group == sp_at // group, here, other_half(here))
    block_of = 2 * (owner ^ sp_at) + (owner != here).astype(jnp.int32)
    named = route_expert[:, :, None] == here[None, None, :]
    hits = jnp.any(named, axis=1)
    earlier = jnp.arange(rows)[:, None] > jnp.arange(rows)[None, :]
    rank = dot(earlier.astype(bf16), hits.astype(bf16)).astype(jnp.int32)
    slot_of = block_of[None, :] * capacity + rank
    slots = jnp.sum(jnp.where(named, slot_of[:, None, :], 0), axis=2)
    slots_t = slots.T
    shares = route_score / jnp.sum(route_score, axis=1, keepdims=True)

    pooled = pooled_blocks(tail, pooled_in, group_map, pool_scale)
    *mine, given = pooled
    mates = flipped(given, "tp", 1)
    parts = []
    for c in range(CHUNKS):
        leaving = projections(
            mine[1:], mates, 1, out_weight, mate_weight, [], c, columns
        )
        parts.append([flipped(v, "tp", 2 * n + 2) for n, v in enumerate(leaving)])
    middles = []
    arrived = [[[] for _ in range(group)] for _ in range(2)]
    for c in range(CHUNKS):
        (own,) = projections(mine[:1], mates, 0, out_weight, mate_weight, [residual], c, columns)
        split = 2 if c == CHUNKS - 1 else 1
        middle, *outgoing = rows_to_send(
            slots_t, own, parts[c], split * group, 2 * capacity // split
        )
        middles.append(middle)
        for k in range(group):
            rows_of = [
                v if k == 0 else flipped(v, "sp", k)
                for v in outgoing[split * k : split * (k + 1)]
            ]
            for side in range(2):
                arrived[side][k].append(rows_of[side % split])

    bit = replicas // 2
    while bit:
        for k, held in list(copied.items()):
            copied[k ^ bit] = [flipped(v, "tp", bit) for v in held]
        bit //= 2
    copied = [v for k in range(replicas) for v in copied[k]]

    def sent_back(made):
        return [made[0]] + [flipped(made[k], "sp", k) for k in range(1, group)]

    made = expert(arrived[0], 0, capacity, norm_gain, (gate_weight, up_weight, down_weight))
    back = sent_back(made)
    made = expert(arrived[1], 1, capacity, norm_gain, copied)
    far_back = sent_back(made)
    total = combined(slots, shares, middles, back, 0, f32)
    return combined(slots, shares, [total], far_back, 1, bf16)


def solution(mesh):
    in_specs = (
        P("sp", "tp"),
        P("tp", None, None),
        P("tp"),
        P("tp", None),
        P(("sp", "tp"), None),
        P(),
        P("sp", None, None),
        P("sp", None, None),
        P("sp", None, None),
        P(("sp", "tp"), None),
        P(("sp", "tp"), None),
    )
    out_specs = P(("sp", "tp"), None)
    return jax.shard_map(body, mesh=mesh, in_specs=in_specs, out_specs=out_specs, check_vma=False)
```

```python
import functools

import jax
import jax.numpy as jnp
from jax import lax
from jax.experimental import pallas as pl
from jax.experimental.pallas import tpu as pltpu
from jax.sharding import PartitionSpec as P


HALO = 16
CHUNKS = 2
CUTS = (0, 2, 4, 6)

f32 = jnp.float32
bf16 = jnp.bfloat16

VMEM = pl.BlockSpec(memory_space=pltpu.VMEM)
SMEM = pl.BlockSpec(memory_space=pltpu.SMEM)
ANY = pl.BlockSpec(memory_space=pl.ANY)


HALVES = [
    (piece, n - a)
    for piece, (a, b) in enumerate(zip(CUTS, CUTS[1:]))
    for n in range(a, b)
]


def dot(a, b):
    return jnp.dot(a, b, preferred_element_type=f32)


def crossed(value, axis, pairs):
    return lax.ppermute(value, axis, pairs)


def flipped(value, axis, bits):
    return crossed(value, axis, [(i, i ^ bits) for i in range(lax.axis_size(axis))])


def reversed_pairs(count):
    return lambda i: (count - 2 - (i // 2) * 2) + i % 2


def cut_kernel(chosen, gate_ref, up_ref, down_ref, x_ref, *rest):
    first = chosen[0] == 0
    outs = dict(zip(chosen, rest[first:-1]))
    sems = rest[-1]
    part = gate_ref.shape[1] // lax.axis_size("tp")
    half = part // 2
    start = lax.axis_index("tp") * part

    def source(n):
        if n < 4:
            at = pl.multiple_of(start + (n % 2) * half, half)
            return (gate_ref if n < 2 else up_ref).at[0, pl.ds(at, half), :]
        at = pl.multiple_of(start, part)
        return down_ref.at[0, (n % 2) * half : (n % 2 + 1) * half, pl.ds(at, part)]

    moves = []
    if first:
        tail = x_ref.at[x_ref.shape[0] - HALO :, :]
        moves.append(pltpu.make_async_copy(tail, rest[0], sems.at[len(HALVES)]))
    for n, (piece, at) in enumerate(HALVES):
        if piece not in outs:
            continue
        target = outs[piece].at[at * half : (at + 1) * half, :]
        moves.append(pltpu.make_async_copy(source(n), target, sems.at[n]))
    for move in moves:
        move.start()
    for move in moves:
        move.wait()


def cut_out(chosen, gate_weight, up_weight, down_weight, pooled_in):
    part = gate_weight.shape[1] // lax.axis_size("tp")
    hidden_units = gate_weight.shape[2]
    assert part == hidden_units
    tail = [jax.ShapeDtypeStruct((HALO, pooled_in.shape[1]), bf16)] * (chosen[0] == 0)
    shapes = tail + [
        jax.ShapeDtypeStruct(((CUTS[n + 1] - CUTS[n]) * part // 2, hidden_units), bf16)
        for n in chosen
    ]
    return pl.pallas_call(
        functools.partial(cut_kernel, chosen),
        in_specs=[ANY] * 4,
        out_specs=[VMEM] * len(shapes),
        out_shape=shapes,
        scratch_shapes=[pltpu.SemaphoreType.DMA((len(HALVES) + 1,))],
        name="cut",
    )(gate_weight, up_weight, down_weight, pooled_in)


def pool_kernel(halo_ref, x_ref, map_ref, scale_ref, *rest):
    *kept_refs, given_ref = rest
    blocks = 2 * len(kept_refs)
    rows = x_ref.shape[0] // blocks
    tp_at = lax.axis_index("tp")
    first = lax.axis_index("sp") * x_ref.shape[0]
    window = jnp.left_shift(jnp.int32(2), tp_at)
    behind = lax.broadcasted_iota(jnp.int32, (rows, rows), 0) - lax.broadcasted_iota(
        jnp.int32, (rows, rows), 1
    )
    band = jnp.where((behind >= 0) & (behind < window), 1.0, 0.0).astype(bf16)
    early = (
        HALO
        + lax.broadcasted_iota(jnp.int32, (HALO, HALO), 0)
        - lax.broadcasted_iota(jnp.int32, (HALO, HALO), 1)
    )
    early_band = jnp.where(early < window, 1.0, 0.0).astype(bf16)
    for k in [*range(1, blocks, 2), *range(0, blocks, 2)]:
        block = tp_at ^ k
        x = x_ref[pl.ds(pl.multiple_of(block * rows, rows), rows), :]
        before = pl.multiple_of(jnp.maximum(block * rows - HALO, 0), HALO)
        tail = jnp.where(block == 0, halo_ref[...], x_ref[pl.ds(before, HALO), :])
        sums = dot(band, x)
        sums = jnp.concatenate([sums[:HALO] + dot(early_band, tail), sums[HALO:]], axis=0)
        position = first + block * rows + lax.broadcasted_iota(jnp.int32, (rows, 1), 0)
        share = 1.0 / jnp.minimum(position + 1, window).astype(f32)
        contrast = (sums * share - x.astype(f32)).astype(bf16)
        pooled = (dot(contrast, map_ref[0]) * scale_ref[...]).astype(bf16)
        if k % 2:
            given_ref[k // 2 * rows : (k // 2 + 1) * rows, :] = pooled
        else:
            kept_refs[k // 2][...] = pooled


def pooled_blocks(tail, pooled_in, group_map, pool_scale):
    rows, width = pooled_in.shape
    replicas = lax.axis_size("tp")
    peers = lax.axis_size("sp")
    halo = crossed(tail, "sp", [(i, i + 1) for i in range(peers - 1)])
    return pl.pallas_call(
        pool_kernel,
        in_specs=[VMEM] * 4,
        out_specs=[VMEM] * (replicas // 2 + 1),
        out_shape=[jax.ShapeDtypeStruct((rows // replicas, width), bf16)] * (replicas // 2)
        + [jax.ShapeDtypeStruct((rows // 2, width), bf16)],
        name="pool",
        compiler_params=pltpu.CompilerParams(vmem_limit_bytes=12 << 20),
    )(halo, pooled_in, group_map, pool_scale[None, :])


def project_kernel(count, *refs):
    mine = refs[:count]
    mates = refs[count : 2 * count]
    w_mine, w_mate = refs[2 * count : 2 * count + 2]
    outs = refs[-count - 1 : -1]
    residual = refs[2 * count + 2 : -count - 1]
    lines = refs[-1]
    rows, width = mine[0].shape

    @pl.when(pl.program_id(0) == 0)
    def _():
        for n in range(count):
            lines[n * rows : (n + 1) * rows, :width] = mine[n][...]
            lines[n * rows : (n + 1) * rows, width:] = mates[n][...]

    sums = dot(lines[:, :width], w_mine[...]) + dot(lines[:, width:], w_mate[...])
    for n in range(count):
        part = sums[n * rows : (n + 1) * rows]
        if residual:
            part = part + residual[0][...].astype(f32)
        outs[n][...] = part.astype(outs[n].dtype)


def projections(mine, mates, first, w_mine, w_mate, residual, chunk, columns):
    count = len(mine)
    rows, width = mine[0].shape
    step = min(512, columns)
    steps = columns // step
    whole = pl.BlockSpec((rows, width), lambda j: (0, 0))
    weight = pl.BlockSpec((width, step), lambda j: (0, chunk * steps + j))
    tile = pl.BlockSpec((rows, step), lambda j: (0, j))
    dtype = f32 if residual else bf16
    return pl.pallas_call(
        functools.partial(project_kernel, count),
        grid=(steps,),
        in_specs=[whole] * count
        + [pl.BlockSpec((rows, width), lambda j, n=n: (first + n, 0)) for n in range(count)]
        + [weight, weight]
        + [pl.BlockSpec((rows, step), lambda j: (0, chunk * steps + j))] * len(residual),
        out_specs=[tile] * count,
        out_shape=[jax.ShapeDtypeStruct((rows, columns), dtype)] * count,
        scratch_shapes=[pltpu.VMEM((count * rows, 2 * width), bf16)],
        name="project",
        compiler_params=pltpu.CompilerParams(vmem_limit_bytes=16 << 20),
    )(*mine, *([mates] * count), w_mine, w_mate, *residual)


def send_kernel(others, slots_ref, own_ref, *refs):
    parts = refs[:others]
    middle_ref, *outs = refs[others:]
    total = own_ref[...]
    for part in parts:
        total = total + part[...].astype(f32)
    middle = total.astype(bf16)
    middle_ref[...] = middle
    length = outs[0].shape[0]
    rows = own_ref.shape[0]
    for k, out in enumerate(outs):
        slot = k * length + lax.broadcasted_iota(jnp.int32, (length, rows), 0)
        hit = slot == slots_ref[0:1, :]
        for j in range(1, slots_ref.shape[0]):
            hit = hit | (slot == slots_ref[j : j + 1, :])
        out[...] = dot(jnp.where(hit, 1.0, 0.0).astype(bf16), middle).astype(bf16)


def rows_to_send(slots_t, own, parts, group, length):
    rows, columns = own.shape
    return pl.pallas_call(
        functools.partial(send_kernel, len(parts)),
        in_specs=[VMEM] * (2 + len(parts)),
        out_specs=[VMEM] * (1 + group),
        out_shape=[jax.ShapeDtypeStruct((rows, columns), bf16)]
        + [jax.ShapeDtypeStruct((length, columns), bf16)] * group,
        name="send",
        compiler_params=pltpu.CompilerParams(vmem_limit_bytes=12 << 20),
    )(slots_t, own, *parts)


def hidden_rows(group, capacity, side, gain_ref, row_refs, lines):
    mine = slice(side * capacity, (side + 1) * capacity)
    chunks = len(row_refs) // group
    for p in range(group):
        blocks = [
            (ref[mine, :] if ref.shape[0] > capacity else ref[...]).astype(f32)
            for ref in row_refs[p * chunks : (p + 1) * chunks]
        ]
        square = sum(jnp.sum(b * b, axis=1, keepdims=True) for b in blocks)
        factor = lax.rsqrt(square / lines.shape[1] + 1e-06)
        at = 0
        for b in blocks:
            span = slice(at, at + b.shape[1])
            lines[p * capacity : (p + 1) * capacity, span] = (
                b * factor * gain_ref[:, span]
            ).astype(bf16)
            at += b.shape[1]


def gated(gate_part, up_part):
    return (gate_part / (1.0 + jnp.exp(-gate_part)) * up_part).astype(bf16)


def own_kernel(group, gain_ref, *refs):
    row_refs, (gate, up, down) = refs[: -group - 4], refs[-group - 4 : -group - 1]
    outs, lines = refs[-group - 1 : -1], refs[-1]
    capacity = outs[0].shape[0]
    hidden_rows(group, capacity, 0, gain_ref, row_refs, lines)
    hidden = gated(dot(lines[...], gate[0]), dot(lines[...], up[0]))
    step = hidden.shape[1]
    for at in range(0, lines.shape[1], step):
        made = dot(hidden, down[0, :, at : at + step]).astype(bf16)
        for p in range(group):
            outs[p][:, at : at + step] = made[p * capacity : (p + 1) * capacity]


def far_hidden_kernel(group, pieces, gain_ref, *refs):
    row_refs, weights = refs[: -2 * pieces - 2], refs[-2 * pieces - 2 : -2]
    out, lines = refs[-2:]
    part = weights[0].shape[0]
    tp_at = lax.axis_index("tp")
    hidden_rows(group, out.shape[0] // group, 1, gain_ref, row_refs, lines)
    gate_part = up_part = 0.0
    for k in range(pieces):
        x = lines[:, pl.ds(pl.multiple_of((tp_at ^ k) * part, part), part)]
        gate_part = gate_part + dot(x, weights[2 * k][...])
        up_part = up_part + dot(x, weights[2 * k + 1][...])
    out[...] = gated(gate_part, up_part)


def far_down_kernel(group, hidden_ref, *refs):
    weights, outs = refs[:-group], refs[-group:]
    capacity = outs[0].shape[0]
    part = weights[0].shape[1]
    inside = lax.axis_index("tp") % len(weights)
    for n, weight in enumerate(weights):
        span = pl.ds(pl.multiple_of((inside ^ n) * part, part), part)
        made = dot(hidden_ref[...], weight[...]).astype(bf16)
        for p in range(group):
            outs[p][:, span] = made[p * capacity : (p + 1) * capacity]


def expert_call(kernel, outs, lines, *operands):
    scratch = [pltpu.VMEM(lines, bf16)] if lines else []
    return pl.pallas_call(
        kernel,
        in_specs=[VMEM] * len(operands),
        out_specs=[VMEM] * len(outs),
        out_shape=[jax.ShapeDtypeStruct(shape, bf16) for shape in outs],
        scratch_shapes=scratch,
        compiler_params=pltpu.CompilerParams(vmem_limit_bytes=24 << 20),
    )(*operands)


def combine_kernel(blocks, half, slots_ref, share_ref, *refs):
    row_refs = refs[: len(blocks)]
    base_refs = refs[len(blocks) : -2]
    out_ref, back = refs[-2:]
    capacity = row_refs[0].shape[0]
    for p in range(len(blocks)):
        back[p * capacity : (p + 1) * capacity, :] = row_refs[p][...]
    shape = (out_ref.shape[0], len(blocks) * capacity)
    slot = blocks[0] * capacity + lax.broadcasted_iota(jnp.int32, shape, 1)
    column = lax.broadcasted_iota(jnp.int32, shape, 1)
    for p in range(1, len(blocks)):
        step = (blocks[p] - blocks[p - 1] - 1) * capacity
        slot = slot + jnp.where(column >= p * capacity, step, 0)
    weigh = jnp.zeros(shape, f32)
    for j in range(slots_ref.shape[1]):
        weigh = weigh + jnp.where(slot == slots_ref[:, j : j + 1], share_ref[:, j : j + 1], 0.0)
    high = weigh.astype(bf16)
    low = (weigh - high.astype(f32)).astype(bf16)
    if half is None:
        at = 0
        for base in base_refs:
            span = slice(at, at + base.shape[1])
            total = base[...].astype(f32) + dot(high, back[:, span]) + dot(low, back[:, span])
            out_ref[:, span] = total.astype(out_ref.dtype)
            at += base.shape[1]
        return
    width = back.shape[1]
    first = lax.axis_index("tp") // (lax.axis_size("tp") // 2)

    def span(n):
        return pl.ds(pl.multiple_of((first ^ n) * width, width), width)

    total = base_refs[0][:, span(half)] + dot(high, back[...]) + dot(low, back[...])
    if half == 0:
        out_ref[...] = total.astype(bf16)
    else:
        out_ref[:, span(0)] = base_refs[1][...]
        out_ref[:, span(1)] = total.astype(bf16)


def combined(slots, shares, bases, returned, half, width, dtype):
    blocks = sorted(returned)
    rows = [returned[n] for n in blocks]
    capacity = rows[0].shape[0]
    return pl.pallas_call(
        functools.partial(combine_kernel, blocks, half),
        in_specs=[VMEM] * (2 + len(rows) + len(bases)),
        out_specs=VMEM,
        out_shape=jax.ShapeDtypeStruct((slots.shape[0], width), dtype),
        scratch_shapes=[pltpu.VMEM((len(rows) * capacity, rows[0].shape[1]), bf16)],
        name="combine",
        compiler_params=pltpu.CompilerParams(vmem_limit_bytes=16 << 20),
    )(slots, shares, *rows, *bases)


def body(
    pooled_in,
    group_map,
    pool_scale,
    out_weight,
    residual,
    norm_gain,
    gate_weight,
    up_weight,
    down_weight,
    route_expert,
    route_score,
):
    experts = lax.axis_size("sp")
    replicas = lax.axis_size("tp")
    sp_at = lax.axis_index("sp")
    rows, width = residual.shape
    top = route_expert.shape[1]
    capacity = max(2, 3 * rows * top // (2 * experts))
    capacity = -(-capacity // 16) * 16
    group = experts // 2
    hidden_units = gate_weight.shape[2]
    other_half = reversed_pairs(experts)
    columns = width // CHUNKS

    mate_weight = flipped(out_weight, "tp", 1)
    tail, *pieces = cut_out([0], gate_weight, up_weight, down_weight, pooled_in)
    rest = list(range(1, len(CUTS) - 1))
    pieces += cut_out(rest, gate_weight, up_weight, down_weight, pooled_in)
    pairs = [(i, other_half(i)) for i in range(experts)]
    copied = {0: [crossed(v, "sp", pairs) for v in pieces]}

    here = jnp.arange(experts, dtype=jnp.int32)
    owner = jnp.where(here // group == sp_at // group, here, other_half(here))
    block_of = 2 * (owner ^ sp_at) + (owner != here).astype(jnp.int32)
    named = route_expert[:, :, None] == here[None, None, :]
    hits = jnp.any(named, axis=1)
    earlier = jnp.arange(rows)[:, None] > jnp.arange(rows)[None, :]
    rank = dot(earlier.astype(bf16), hits.astype(bf16)).astype(jnp.int32)
    slot_of = block_of[None, :] * capacity + rank
    slots = jnp.sum(jnp.where(named, slot_of[:, None, :], 0), axis=2)
    slots_t = slots.T
    shares = route_score / jnp.sum(route_score, axis=1, keepdims=True)

    pooled = pooled_blocks(tail, pooled_in, group_map, pool_scale)
    *mine, given = pooled
    mates = flipped(given, "tp", 1)
    parts = []
    for c in range(CHUNKS):
        leaving = projections(
            mine[1:], mates, 1, out_weight, mate_weight, [], c, columns
        )
        parts.append([flipped(v, "tp", 2 * n + 2) for n, v in enumerate(leaving)])
    middles = []
    arrived = [[[] for _ in range(group)] for _ in range(2)]
    for c in range(CHUNKS):
        (own,) = projections(
            mine[:1], mates, 0, out_weight, mate_weight, [residual], c, columns
        )
        split = 2
        middle, *outgoing = rows_to_send(
            slots_t, own, parts[c], split * group, 2 * capacity // split
        )
        middles.append(middle)
        for k in range(group):
            rows_of = [
                v if k == 0 else flipped(v, "sp", k)
                for v in outgoing[split * k : split * (k + 1)]
            ]
            for side in range(2):
                arrived[side][k].append(rows_of[side % split])

    bit = replicas // 2
    while bit:
        for k, held in list(copied.items()):
            copied[k ^ bit] = [flipped(v, "tp", bit) for v in held]
        bit //= 2

    def sent_back(side, made):
        back = {2 * k + side: flipped(made[k], "sp", k) for k in range(1, group)}
        return {side: made[0]} | back

    gain = norm_gain[None, :]
    lines = (group * capacity, width)
    flat = [[v for blocks in side for v in blocks] for side in arrived]
    made = expert_call(
        functools.partial(own_kernel, group),
        [(capacity, width)] * group,
        lines,
        gain,
        *flat[0],
        gate_weight,
        up_weight,
        down_weight,
    )
    back = sent_back(0, made)
    (hidden,) = expert_call(
        functools.partial(far_hidden_kernel, group, replicas),
        [(group * capacity, hidden_units)],
        lines,
        gain,
        *flat[1],
        *[v for k in range(replicas) for v in copied[k][:2]],
    )
    far_back = []
    for n in range(2):
        ks = range(n * replicas // 2, (n + 1) * replicas // 2)
        made = expert_call(
            functools.partial(far_down_kernel, group),
            [(capacity, width // 2)] * group,
            None,
            hidden,
            *[copied[k][2] for k in ks],
        )
        far_back.append(sent_back(1, made))
    total = combined(slots, shares, middles, back, None, width, f32)
    first = combined(slots, shares, [total], far_back[0], 0, width // 2, bf16)
    return combined(slots, shares, [total, first], far_back[1], 1, width, bf16)


def solution(mesh):
    in_specs = (
        P("sp", "tp"),
        P("tp", None, None),
        P("tp"),
        P("tp", None),
        P(("sp", "tp"), None),
        P(),
        P("sp", None, None),
        P("sp", None, None),
        P("sp", None, None),
        P(("sp", "tp"), None),
        P(("sp", "tp"), None),
    )
    out_specs = P(("sp", "tp"), None)
    return jax.shard_map(
        body, mesh=mesh, in_specs=in_specs, out_specs=out_specs, check_vma=False
    )
```
